32 devices in a mesh: grp: 2 (over y), fs: 4 (over z), tp: 4 (over x, core).
Axes of the slice: x: 2, y: 2, z: 4, core: 2. Of those that a mesh axis runs over, the one named last changes fastest.
Arguments:
- tokens: bfloat16 [3072, 2048], P(('grp', 'fs'), 'tp'), parts along dimension 0, may hold values from -6 to 6
- mix_gain: float32 [2048], replicated, may hold values from 0.1 to 1.9
- w_signal: bfloat16 [2048, 1024], P('fs', 'tp'), may hold values from -0.125 to 0.125
- w_outer_gate: bfloat16 [2048, 1024], P('fs', 'tp'), may hold values from -0.125 to 0.125
- w_inner_gate: bfloat16 [2048, 1024], P('fs', 'tp'), may hold values from -0.125 to 0.125
- mix_taps: float32 [3, 1024], P(None, 'tp'), may hold values from -3 to 3
- w_mix_out: bfloat16 [1024, 2048], P('tp', 'fs'), may hold values from -0.1875 to 0.1875
- ffn_gain: float32 [2048], replicated, may hold values from 0.1 to 1.9
- w_gate: bfloat16 [2048, 5120], P('fs', 'tp'), may hold values from -0.125 to 0.125
- w_value: bfloat16 [2048, 5120], P('fs', 'tp'), may hold values from -0.125 to 0.125
- up_taps: float32 [2, 3, 5120], P(None, None, 'tp'), may hold values from -3 to 3
- up_bias: float32 [2, 5120], P(None, 'tp'), may hold values from -3 to 3
- w_down: bfloat16 [5120, 2048], P('tp', 'fs'), may hold values from -0.078125 to 0.078125
Outputs:
- layer_out: bfloat16 [3072, 2048], P(('grp', 'fs'), 'tp'), parts along dimension 0
The draws below stay inside these ranges and needn't reach their ends.
There are 2 independent parts, one for each index of `grp`. The reference program is written for one: setup_inputs(seed, part) draws one part's arguments, and reference() takes and returns one part's arrays. A program takes and returns all parts, laid end to end along the dimension named above; an argument that names none is the same for every part. Nothing has to cross between parts.
All inputs are finite; a program needn't handle non-finite values.
Results may differ from the reference program's by a relative error of at most 0.022.
Values may be sent and summed in bfloat16 or wider, within the bound.
A program may use at most 64 MiB of HBM per device.

```python
import jax
import jax.numpy as jnp
from jax import lax

D = 2048
DC = 1024
FF = 5120
TAPS = 3
LEN = 192
TOKENS = 1536
N_TP = 4


def block_levels(stream_key, extent, split, least, high):
    level, own = 1.0, jax.random.fold_in(stream_key, 6)
    for dim, blocks in split:
        steps = jnp.exp(jax.random.uniform(jax.random.fold_in(own, dim), (blocks,), jnp.float32, least / len(split), high / len(split)))
        level = level * jnp.repeat(steps, extent[dim] // blocks).reshape([-1 if axis == dim else 1 for axis in range(len(extent))])
    return level


def centred(rng, dims, deviation, bound, shards=(), dtype=jnp.bfloat16):
    drawn = jax.random.normal(rng, dims, jnp.float32) * deviation
    if len(shards) > 0:
        drawn = block_levels(rng, dims, shards, -0.22, 0.18) * drawn
    return jnp.clip(drawn, min=-bound, max=bound).astype(dtype)


def setup_inputs(seed: int = 0, part: int = 0) -> dict:
    key_list = jax.random.split(jax.random.key(seed), 14)
    part_splits = jax.random.split(jax.random.fold_in(key_list[13], part), 14)
    return {
        "tokens": centred(part_splits[0], (TOKENS, D), 1.0, 6.0, ((0, 4), (1, 4))),
        "mix_gain": jnp.clip(1.0 + 0.18 * jax.random.normal(key_list[1], (D,), jnp.float32), 0.1, 1.9),
        "w_signal": centred(key_list[2], (D, DC), D ** -0.5, 0.125, ((0, 4), (1, 4))),
        "w_outer_gate": centred(key_list[3], (D, DC), D ** -0.5, 0.125, ((0, 4), (1, 4))),
        "w_inner_gate": centred(key_list[4], (D, DC), D ** -0.5, 0.125, ((0, 4), (1, 4))),
        "mix_taps": centred(key_list[5], (TAPS, DC), 0.577, 3.0, ((1, 4),), jnp.float32),
        "w_mix_out": centred(key_list[6], (DC, D), DC ** -0.5, 0.1875, ((0, 4), (1, 4))),
        "ffn_gain": jnp.clip(1.0 + 0.18 * jax.random.normal(key_list[7], (D,), jnp.float32), 0.1, 1.9),
        "w_gate": centred(key_list[8], (D, FF), D ** -0.5, 0.125, ((0, 4), (1, 4))),
        "w_value": centred(key_list[9], (D, FF), D ** -0.5, 0.125, ((0, 4), (1, 4))),
        "up_taps": centred(key_list[10], (2, TAPS, FF), 0.577, 3.0, ((2, 4),), jnp.float32),
        "up_bias": centred(key_list[11], (2, FF), 0.5, 3.0, ((1, 4),), jnp.float32),
        "w_down": centred(key_list[12], (FF, D), FF ** -0.5, 0.078125, ((0, 4), (1, 4))),
    }


def conv_positions(values, taps):
    width = values.shape[1]
    blocks = values.reshape(-1, LEN, width)
    padded = jnp.pad(blocks, ((0, 0), (2, 0), (0, 0)))
    result = padded[:, 0:LEN] * taps[0] + padded[:, 1:LEN + 1] * taps[1] + padded[:, 2:LEN + 2] * taps[2]
    return result.reshape(-1, width)

def rms_norm(stream, gain):
    values = stream.astype(jnp.float32)
    scale = lax.rsqrt(lax.optimization_barrier(jnp.mean(values * values, axis=-1, keepdims=True)) + 1e-06)
    return (values * scale * gain).astype(jnp.bfloat16)

def block_partials(left, right, blocks):
    width = left.shape[1] // blocks
    total = jnp.zeros((left.shape[0], right.shape[1]), jnp.float32)
    for index in range(blocks):
        part = jnp.dot(left[:, index * width:(index + 1) * width], right[index * width:(index + 1) * width], preferred_element_type=jnp.float32)
        part = lax.optimization_barrier(part.astype(jnp.bfloat16))
        total = total + part.astype(jnp.float32)
    return total

def reference(tokens, mix_gain, w_signal, w_outer_gate, w_inner_gate, mix_taps, w_mix_out, ffn_gain, w_gate, w_value, up_taps, up_bias, w_down):
    normed = rms_norm(tokens, mix_gain)
    signal = jnp.dot(normed, w_signal, preferred_element_type=jnp.float32).astype(jnp.bfloat16)
    outer = jnp.dot(normed, w_outer_gate, preferred_element_type=jnp.float32).astype(jnp.bfloat16)
    inner = jnp.dot(normed, w_inner_gate, preferred_element_type=jnp.float32).astype(jnp.bfloat16)
    product = inner.astype(jnp.float32) * signal.astype(jnp.float32)
    mixed = (outer.astype(jnp.float32) * conv_positions(product, mix_taps)).astype(jnp.bfloat16)
    mix_sum = block_partials(mixed, w_mix_out, N_TP)
    resid = (tokens.astype(jnp.float32) + mix_sum).astype(jnp.bfloat16)
    normed_ffn = rms_norm(resid, ffn_gain)
    gate = jnp.dot(normed_ffn, w_gate, preferred_element_type=jnp.float32).astype(jnp.bfloat16)
    value = jnp.dot(normed_ffn, w_value, preferred_element_type=jnp.float32).astype(jnp.bfloat16)
    gate_conv = conv_positions(gate.astype(jnp.float32), up_taps[0]) + up_bias[0]
    value_conv = conv_positions(value.astype(jnp.float32), up_taps[1]) + up_bias[1]
    hidden = (jax.nn.silu(gate_conv) * value_conv).astype(jnp.bfloat16)
    ffn_sum = block_partials(hidden, w_down, N_TP)
    return (resid.astype(jnp.float32) + ffn_sum).astype(jnp.bfloat16)
```

```python
import functools

import jax
import jax.numpy as jnp
from jax import lax
from jax.experimental import pallas as pl
from jax.experimental.pallas import tpu as pltpu
from jax.sharding import PartitionSpec as P

SEQS_DEV = 2


def conv_positions(values, taps):
    width = values.shape[1]
    blocks = values.reshape(SEQS_DEV, -1, width)
    length = blocks.shape[1]
    padded = jnp.pad(blocks, ((0, 0), (2, 0), (0, 0)))
    result = (
        padded[:, 0:length] * taps[0]
        + padded[:, 1 : length + 1] * taps[1]
        + padded[:, 2 : length + 2] * taps[2]
    )
    return result.reshape(-1, width)


def rms_norm(stream, gain):
    values = stream.astype(jnp.float32)
    scale = lax.rsqrt(jnp.mean(values * values, axis=-1, keepdims=True) + 1e-06)
    return (values * scale * gain).astype(jnp.bfloat16)


def on_device(
    tokens,
    mix_gain,
    w_signal,
    w_outer_gate,
    w_inner_gate,
    mix_taps,
    w_mix_out,
    ffn_gain,
    w_gate,
    w_value,
    up_taps,
    up_bias,
    w_down,
):
    whole = lax.all_gather(tokens, "tp", axis=1, tiled=True)
    normed = rms_norm(whole, mix_gain)
    pieces = (
        lax.all_gather(w_signal, "fs", axis=0, tiled=True),
        lax.all_gather(w_outer_gate, "fs", axis=0, tiled=True),
        lax.all_gather(w_inner_gate, "fs", axis=0, tiled=True),
    )
    columns = normed
    signal, outer, inner = tuple(
        (jnp.dot(columns, piece, preferred_element_type=jnp.float32) for piece in pieces)
    )
    signal = signal.astype(jnp.bfloat16).astype(jnp.float32)
    outer = outer.astype(jnp.bfloat16).astype(jnp.float32)
    inner = inner.astype(jnp.bfloat16).astype(jnp.float32)
    mixed = (outer * conv_positions(inner * signal, mix_taps)).astype(jnp.bfloat16)
    mix_terms = jnp.dot(
        mixed,
        lax.all_gather(w_mix_out, "fs", axis=1, tiled=True),
        preferred_element_type=jnp.float32,
    )
    mix_sum = lax.psum_scatter(
        mix_terms.astype(jnp.bfloat16), "tp", scatter_dimension=1, tiled=True
    ).astype(jnp.float32)
    resid = (tokens.astype(jnp.float32) + mix_sum).astype(jnp.bfloat16)
    whole_ffn = lax.all_gather(resid, "tp", axis=1, tiled=True)
    normed_ffn = rms_norm(whole_ffn, ffn_gain)
    pieces = (
        lax.all_gather(w_gate, "fs", axis=0, tiled=True),
        lax.all_gather(w_value, "fs", axis=0, tiled=True),
    )
    columns = normed_ffn
    gate = jnp.dot(columns, pieces[0], preferred_element_type=jnp.float32)
    value = jnp.dot(columns, pieces[1], preferred_element_type=jnp.float32)
    gate = gate.astype(jnp.bfloat16).astype(jnp.float32)
    value = value.astype(jnp.bfloat16).astype(jnp.float32)
    gate_conv = conv_positions(gate, up_taps[0]) + up_bias[0]
    value_conv = conv_positions(value, up_taps[1]) + up_bias[1]
    hidden = (jax.nn.silu(gate_conv) * value_conv).astype(jnp.bfloat16)
    ffn_terms = jnp.dot(
        hidden, lax.all_gather(w_down, "fs", axis=1, tiled=True), preferred_element_type=jnp.float32
    )
    ffn_sum = lax.psum_scatter(
        ffn_terms.astype(jnp.bfloat16), "tp", scatter_dimension=1, tiled=True
    ).astype(jnp.float32)
    return (resid.astype(jnp.float32) + ffn_sum).astype(jnp.bfloat16)


MESH = pl.DeviceIdType.MESH
UP, DOWN = 0, 1


def shifted(values, by, length):
    rolled = pltpu.roll(values, by, 0)
    position = lax.rem(lax.broadcasted_iota(jnp.int32, values.shape, 0), length)
    return jnp.where(position < by, 0.0, rolled)


def conv_rows(values, taps, length):
    return (
        shifted(values, 2, length) * taps[0:1]
        + shifted(values, 1, length) * taps[1:2]
        + values * taps[2:3]
    )


def layer_kernel(
    n_fs,
    n_tp,
    tokens,
    mix_gain,
    w_signal,
    w_outer_gate,
    w_inner_gate,
    mix_taps,
    w_mix_out,
    ffn_gain,
    w_gate,
    w_value,
    up_taps,
    up_bias,
    w_down,
    out,
    mix_in,
    mix_out,
    ffn_in,
    ffn_out,
    tok,
    res,
    normed,
    total,
    part,
    got,
    part_ffn,
    got_ffn,
    z_send,
    z_recv,
    y_send,
    y_recv,
    load_sem,
    tp_send,
    tp_recv,
):
    g, j, k = lax.axis_index("grp"), lax.axis_index("fs"), lax.axis_index("tp")
    rows, own_cols = tokens.shape
    length = rows // SEQS_DEV
    shard, chans = w_signal.shape
    half, half_chans = shard // 2, chans // 2
    stages = 1 + w_gate.shape[1] // chans

    def views(s, source, side):
        at_rows = pl.ds(pl.multiple_of((source * 2 + side) * half, half), half)
        at_chans = pl.ds(pl.multiple_of(side * half_chans, half_chans), half_chans)
        if isinstance(s, int) and s == 0:
            return mix_in.at[:, at_rows, :], mix_out.at[source, at_chans, :]
        return ffn_in.at[s - 1, :, at_rows, :], ffn_out.at[s - 1, source, at_chans, :]

    def z_copies(s, source, way):
        to = j + 1 if way == UP else j - 1
        return [
            pltpu.make_async_remote_copy(
                src_ref=view,
                dst_ref=view,
                send_sem=z_send.at[way, 2 * s + p, source],
                recv_sem=z_recv.at[2 * s + p, source],
                device_id={"fs": to},
                device_id_type=MESH,
            )
            for p, view in enumerate(views(s, source, g))
        ]

    def y_copies(s, source, side):
        return [
            pltpu.make_async_remote_copy(
                src_ref=view,
                dst_ref=view,
                send_sem=y_send.at[2 * s + p, source],
                recv_sem=y_recv.at[2 * s + p, source],
                device_id={"grp": 1 - g},
                device_id_type=MESH,
            )
            for p, view in enumerate(views(s, source, side))
        ]

    def start(copies):
        for copy in copies:
            copy.start()

    def own(s, way):
        start(z_copies(s, j, way))

    def relay(s, last):
        for d in range(1, n_fs):

            @pl.when(j - d >= 0)
            def _():
                for copy in z_copies(s, j - d, UP):
                    copy.wait_recv()

                @pl.when(j + 1 < n_fs)
                def _():
                    start(z_copies(s, j - d, UP))

                start(y_copies(s, j - d, g))

            @pl.when(j + d < n_fs)
            def _():
                for copy in z_copies(s, j + d, DOWN):
                    copy.wait_recv()

                @pl.when(j >= 1)
                def _():
                    start(z_copies(s, j + d, DOWN))

                start(y_copies(s, j + d, g))

            if not last:

                @pl.when((j == d) & (j + 1 < n_fs))
                def _():
                    own(s + 1, UP)

                @pl.when((n_fs - 1 - j == d) & (j >= 1))
                def _():
                    own(s + 1, DOWN)

    def arrived(s):
        for d in range(1, n_fs):
            for copy in y_copies(s, lax.rem(j + d, n_fs), 1 - g):
                copy.wait_recv()

    def tp_copy(phase, d, src, dst, to):
        return pltpu.make_async_remote_copy(
            src_ref=src,
            dst_ref=dst,
            send_sem=tp_send.at[phase, d],
            recv_sem=tp_recv.at[phase, d],
            device_id={"tp": to},
            device_id_type=MESH,
        )

    def gather_copy(phase, buffer, d):
        return tp_copy(phase, d, buffer.at[k], buffer.at[k], lax.rem(k + d, n_tp))

    def gather_wait(phase, buffer, d):
        source = lax.rem(k + n_tp - d, n_tp)
        tp_copy(phase, d, buffer.at[source], buffer.at[source], lax.rem(k + d, n_tp)).wait_recv()

    def scatter_copy(phase, sent, received, d):
        to = lax.rem(k + d, n_tp)
        return tp_copy(phase, d, sent.at[to], received.at[d], to)

    barrier = pltpu.get_barrier_semaphore()
    for peer in (lax.rem(j + 1, n_fs), lax.rem(j + n_fs - 1, n_fs)):
        pl.semaphore_signal(barrier, inc=1, device_id={"fs": peer}, device_id_type=MESH)
    pl.semaphore_signal(barrier, inc=1, device_id={"grp": 1 - g}, device_id_type=MESH)
    for d in range(1, n_tp):
        pl.semaphore_signal(
            barrier, inc=1, device_id={"tp": lax.rem(k + d, n_tp)}, device_id_type=MESH
        )

    at_rows = pl.ds(pl.multiple_of(j * shard, shard), shard)
    loads = [
        pltpu.make_async_copy(ref, mix_in.at[i, at_rows, :], load_sem.at[i])
        for i, ref in enumerate((w_signal, w_outer_gate, w_inner_gate))
    ]
    loads.append(pltpu.make_async_copy(w_mix_out, mix_out.at[j], load_sem.at[3]))
    loads.append(pltpu.make_async_copy(tokens, tok.at[k], load_sem.at[4]))
    for s in range(1, stages):
        cut = pl.ds((s - 1) * chans, chans)
        base = 5 + 3 * (s - 1)
        loads.append(
            pltpu.make_async_copy(
                w_gate.at[:, cut], ffn_in.at[s - 1, 0, at_rows, :], load_sem.at[base]
            )
        )
        loads.append(
            pltpu.make_async_copy(
                w_value.at[:, cut], ffn_in.at[s - 1, 1, at_rows, :], load_sem.at[base + 1]
            )
        )
        loads.append(
            pltpu.make_async_copy(
                w_down.at[cut, :], ffn_out.at[s - 1, j], load_sem.at[base + 2]
            )
        )
    start(loads)
    for copy in loads[:5]:
        copy.wait()
    pl.semaphore_wait(barrier, 3 + n_tp - 1)

    @pl.when(j + 1 < n_fs)
    def _():
        own(0, UP)

    @pl.when(j >= 1)
    def _():
        own(0, DOWN)

    for d in range(1, n_tp):
        gather_copy(0, tok, d).start()
    for copy in loads[5:]:
        copy.wait()

    @pl.when(j == 0)
    def _():
        for s in range(1, stages):
            own(s, UP)

    @pl.when(j == n_fs - 1)
    def _():
        for s in range(1, stages):
            own(s, DOWN)

    def norm(buffer, gain):
        squares = jnp.zeros((rows, 1), jnp.float32)
        for b in range(n_tp):
            values = buffer[b].astype(jnp.float32)
            squares = squares + jnp.sum(values * values, axis=-1, keepdims=True)
        scale = lax.rsqrt(squares / (n_tp * own_cols) + 1e-06)
        for b in range(n_tp):
            cut = slice(b * own_cols, (b + 1) * own_cols)
            values = buffer[b].astype(jnp.float32)
            normed[:, cut] = (values * scale * gain[:, cut]).astype(jnp.bfloat16)

    for d in range(1, n_tp):
        gather_wait(0, tok, d)
    norm(tok, mix_gain)

    relay(0, False)
    relay(1, False)
    arrived(0)

    def project(weight):
        product = jnp.dot(normed[...], weight, preferred_element_type=jnp.float32)
        return product.astype(jnp.bfloat16).astype(jnp.float32)

    gated = project(mix_in[2]) * project(mix_in[0])
    conv = conv_rows(gated, mix_taps[...], length)
    mixed = (project(mix_in[1]) * conv).astype(jnp.bfloat16)
    for b in range(n_fs):
        total[:, b * shard : (b + 1) * shard] = jnp.dot(
            mixed, mix_out[b], preferred_element_type=jnp.float32
        )
    for b in range(n_tp):
        part[b] = total[:, b * own_cols : (b + 1) * own_cols].astype(jnp.bfloat16)
    for d in range(1, n_tp):
        scatter_copy(1, part, got, d).start()

    relay(2, False)

    def summed(phase, sent, received):
        value = sent[k].astype(jnp.float32)
        for d in range(1, n_tp):
            scatter_copy(phase, sent, received, d).wait_recv()
            value = value + received[d].astype(jnp.float32)
        return value

    res[k] = (tok[k].astype(jnp.float32) + summed(1, part, got)).astype(jnp.bfloat16)
    for d in range(1, n_tp):
        gather_copy(2, res, d).start()

    relay(3, stages == 4)
    for d in range(1, n_tp):
        gather_wait(2, res, d)
    norm(res, ffn_gain)
    total[...] = jnp.zeros_like(total)

    def feed(s):
        arrived(s)
        cut = pl.ds(pl.multiple_of((s - 1) * chans, chans), chans)
        gate = conv_rows(project(ffn_in[s - 1, 0]), up_taps[0, :, cut], length) + up_bias[0:1, cut]
        value = conv_rows(project(ffn_in[s - 1, 1]), up_taps[1, :, cut], length) + up_bias[1:2, cut]
        hidden = (gate / (1.0 + jnp.exp(-gate)) * value).astype(jnp.bfloat16)
        for b in range(n_fs):
            total[:, b * shard : (b + 1) * shard] += jnp.dot(
                hidden, ffn_out[s - 1, b], preferred_element_type=jnp.float32
            )

    @pl.loop(1, stages)
    def _(s):
        @pl.when(s + 3 < stages - 1)
        def _():
            relay(s + 3, False)

        @pl.when(s + 3 == stages - 1)
        def _():
            relay(s + 3, True)

        feed(s)

    for b in range(n_tp):
        part_ffn[b] = total[:, b * own_cols : (b + 1) * own_cols].astype(jnp.bfloat16)
    for d in range(1, n_tp):
        scatter_copy(3, part_ffn, got_ffn, d).start()
    out[...] = (res[k].astype(jnp.float32) + summed(3, part_ffn, got_ffn)).astype(jnp.bfloat16)

    for d in range(1, n_tp):
        gather_copy(0, tok, d).wait_send()
        scatter_copy(1, part, got, d).wait_send()
        gather_copy(2, res, d).wait_send()
        scatter_copy(3, part_ffn, got_ffn, d).wait_send()

    def drain(s):
        for d in range(n_fs):

            @pl.when((j - d >= 0) & (j + 1 < n_fs))
            def _():
                for copy in z_copies(s, j - d, UP):
                    copy.wait_send()

            @pl.when((j + d < n_fs) & (j >= 1))
            def _():
                for copy in z_copies(s, j + d, DOWN):
                    copy.wait_send()

        for d in range(1, n_fs):
            for copy in y_copies(s, lax.rem(j + d, n_fs), g):
                copy.wait_send()

    drain(0)
    pl.loop(1, stages)(drain)


def fused(n_fs, n_tp, *args):
    tokens, w_signal, w_gate = args[0], args[2], args[8]
    rows, cols = tokens.shape
    shard, chans = w_signal.shape
    stages = 1 + w_gate.shape[1] // chans
    width = n_fs * shard
    args = list(args)
    args[1], args[7] = args[1].reshape(1, -1), args[7].reshape(1, -1)
    in_vmem = {1, 5, 7, 10, 11}
    wide = (n_tp, rows, cols)
    copies = 2 * stages
    dma = pltpu.SemaphoreType.DMA
    return pl.pallas_call(
        functools.partial(layer_kernel, n_fs, n_tp),
        out_shape=jax.ShapeDtypeStruct((rows, cols), jnp.bfloat16),
        in_specs=[
            pl.BlockSpec(memory_space=pltpu.VMEM if i in in_vmem else pl.ANY)
            for i in range(len(args))
        ],
        out_specs=pl.BlockSpec(memory_space=pltpu.VMEM),
        scratch_shapes=[
            pltpu.VMEM((3, width, chans), jnp.bfloat16),
            pltpu.VMEM((n_fs, chans, shard), jnp.bfloat16),
            pltpu.VMEM((stages - 1, 2, width, chans), jnp.bfloat16),
            pltpu.VMEM((stages - 1, n_fs, chans, shard), jnp.bfloat16),
            pltpu.VMEM(wide, jnp.bfloat16),
            pltpu.VMEM(wide, jnp.bfloat16),
            pltpu.VMEM((rows, width), jnp.bfloat16),
            pltpu.VMEM((rows, width), jnp.float32),
            pltpu.VMEM(wide, jnp.bfloat16),
            pltpu.VMEM(wide, jnp.bfloat16),
            pltpu.VMEM(wide, jnp.bfloat16),
            pltpu.VMEM(wide, jnp.bfloat16),
            dma((2, copies, n_fs)),
            dma((copies, n_fs)),
            dma((copies, n_fs)),
            dma((copies, n_fs)),
            dma((5 + 3 * (stages - 1),)),
            dma((4, n_tp)),
            dma((4, n_tp)),
        ],
        compiler_params=pltpu.CompilerParams(
            collective_id=0, has_side_effects=True, vmem_limit_bytes=60 * 1024 * 1024
        ),
    )(*args)


def solution(mesh):
    n_fs, n_tp = mesh.shape["fs"], mesh.shape["tp"]
    body = functools.partial(fused, n_fs, n_tp)
    if n_fs > 8 or mesh.shape["grp"] != 2:
        body = on_device
    placed = (
        P(("grp", "fs"), "tp"),
        P(),
        P("fs", "tp"),
        P("fs", "tp"),
        P("fs", "tp"),
        P(None, "tp"),
        P("tp", "fs"),
        P(),
        P("fs", "tp"),
        P("fs", "tp"),
        P(None, None, "tp"),
        P(None, "tp"),
        P("tp", "fs"),
    )
    return jax.shard_map(
        body, mesh=mesh, in_specs=placed, out_specs=P(("grp", "fs"), "tp"), check_vma=False
    )
```

```python
import functools

import jax
import jax.numpy as jnp
from jax import lax
from jax.experimental import pallas as pl
from jax.experimental.pallas import tpu as pltpu
from jax.sharding import PartitionSpec as P

SEQS_DEV = 2


def conv_positions(values, taps):
    width = values.shape[1]
    blocks = values.reshape(SEQS_DEV, -1, width)
    length = blocks.shape[1]
    padded = jnp.pad(blocks, ((0, 0), (2, 0), (0, 0)))
    result = (
        padded[:, 0:length] * taps[0]
        + padded[:, 1 : length + 1] * taps[1]
        + padded[:, 2 : length + 2] * taps[2]
    )
    return result.reshape(-1, width)


def rms_norm(stream, gain):
    values = stream.astype(jnp.float32)
    scale = lax.rsqrt(jnp.mean(values * values, axis=-1, keepdims=True) + 1e-06)
    return (values * scale * gain).astype(jnp.bfloat16)


def on_device(
    tokens,
    mix_gain,
    w_signal,
    w_outer_gate,
    w_inner_gate,
    mix_taps,
    w_mix_out,
    ffn_gain,
    w_gate,
    w_value,
    up_taps,
    up_bias,
    w_down,
):
    whole = lax.all_gather(tokens, "tp", axis=1, tiled=True)
    normed = rms_norm(whole, mix_gain)
    pieces = (
        lax.all_gather(w_signal, "fs", axis=0, tiled=True),
        lax.all_gather(w_outer_gate, "fs", axis=0, tiled=True),
        lax.all_gather(w_inner_gate, "fs", axis=0, tiled=True),
    )
    columns = normed
    signal, outer, inner = tuple(
        (jnp.dot(columns, piece, preferred_element_type=jnp.float32) for piece in pieces)
    )
    signal = signal.astype(jnp.bfloat16).astype(jnp.float32)
    outer = outer.astype(jnp.bfloat16).astype(jnp.float32)
    inner = inner.astype(jnp.bfloat16).astype(jnp.float32)
    mixed = (outer * conv_positions(inner * signal, mix_taps)).astype(jnp.bfloat16)
    mix_terms = jnp.dot(
        mixed,
        lax.all_gather(w_mix_out, "fs", axis=1, tiled=True),
        preferred_element_type=jnp.float32,
    )
    mix_sum = lax.psum_scatter(
        mix_terms.astype(jnp.bfloat16), "tp", scatter_dimension=1, tiled=True
    ).astype(jnp.float32)
    resid = (tokens.astype(jnp.float32) + mix_sum).astype(jnp.bfloat16)
    whole_ffn = lax.all_gather(resid, "tp", axis=1, tiled=True)
    normed_ffn = rms_norm(whole_ffn, ffn_gain)
    pieces = (
        lax.all_gather(w_gate, "fs", axis=0, tiled=True),
        lax.all_gather(w_value, "fs", axis=0, tiled=True),
    )
    columns = normed_ffn
    gate = jnp.dot(columns, pieces[0], preferred_element_type=jnp.float32)
    value = jnp.dot(columns, pieces[1], preferred_element_type=jnp.float32)
    gate = gate.astype(jnp.bfloat16).astype(jnp.float32)
    value = value.astype(jnp.bfloat16).astype(jnp.float32)
    gate_conv = conv_positions(gate, up_taps[0]) + up_bias[0]
    value_conv = conv_positions(value, up_taps[1]) + up_bias[1]
    hidden = (jax.nn.silu(gate_conv) * value_conv).astype(jnp.bfloat16)
    ffn_terms = jnp.dot(
        hidden, lax.all_gather(w_down, "fs", axis=1, tiled=True), preferred_element_type=jnp.float32
    )
    ffn_sum = lax.psum_scatter(
        ffn_terms.astype(jnp.bfloat16), "tp", scatter_dimension=1, tiled=True
    ).astype(jnp.float32)
    return (resid.astype(jnp.float32) + ffn_sum).astype(jnp.bfloat16)


MESH = pl.DeviceIdType.MESH
UP, DOWN = 0, 1
LANES = 128


def shifted(values, by, length):
    rolled = pltpu.roll(values, by, 0)
    position = lax.rem(lax.broadcasted_iota(jnp.int32, values.shape, 0), length)
    return jnp.where(position < by, 0.0, rolled)


def conv_rows(values, taps, length):
    return (
        shifted(values, 2, length) * taps[0:1]
        + shifted(values, 1, length) * taps[1:2]
        + values * taps[2:3]
    )


def layer_kernel(
    n_fs,
    n_tp,
    tokens,
    mix_gain,
    w_signal,
    w_outer_gate,
    w_inner_gate,
    mix_taps,
    w_mix_out,
    ffn_gain,
    w_gate,
    w_value,
    up_taps,
    up_bias,
    w_down,
    out,
    mix_in,
    mix_out,
    ffn_in,
    ffn_out,
    tok,
    res,
    normed,
    total,
    part,
    got,
    part_ffn,
    got_core,
    sum_x,
    got_x,
    sum_z,
    got_z,
    z_send,
    z_recv,
    y_send,
    y_recv,
    load_sem,
    tp_send,
    tp_recv,
    all_send,
    all_recv,
    core_send,
    core_recv,
    x_send,
    x_recv,
    pair_send,
    pair_recv,
):
    g, j, k = lax.axis_index("grp"), lax.axis_index("fs"), lax.axis_index("tp")
    rows, own_cols = tokens.shape
    length = rows // SEQS_DEV
    shard, chans = w_signal.shape
    half = shard // 2
    hidden_half = w_gate.shape[1] // 2
    stages = 1 + hidden_half // LANES
    n_x = n_tp // 2
    x, c = k // 2, lax.rem(k, 2)
    core = k + 1 - 2 * c
    p = lax.rem(j, 2)
    pair = j + 1 - 2 * p
    mine = pl.ds(pl.multiple_of(p * rows, rows), rows)
    theirs = pl.ds(pl.multiple_of((1 - p) * rows, rows), rows)

    def chunks(s):
        return (None,) if isinstance(s, int) and s == 0 else (0, 1)

    def top(q):
        return n_fs - 1 if q is None or (n_fs - 1) % 2 == q else n_fs - 2

    def bottom(q):
        return 0 if q is None else q

    def views(s, q, source, side):
        at_rows = pl.ds(pl.multiple_of((source * 2 + side) * half, half), half)
        tall = chans // 2 if q is None else LANES // 2
        at_chans = pl.ds(pl.multiple_of(side * tall, tall), tall)
        if q is None:
            return mix_in.at[:, at_rows, :], mix_out.at[source, at_chans, :]
        return ffn_in.at[s - 1, q, at_rows, :], ffn_out.at[s - 1, q, source, at_chans, :]

    def slot(s, q, i):
        return i if q is None else 2 + (s - 1) * 4 + q * 2 + i

    def z_copies(s, q, source, way):
        return [
            pltpu.make_async_remote_copy(
                src_ref=view,
                dst_ref=view,
                send_sem=z_send.at[way, slot(s, q, i), source],
                recv_sem=z_recv.at[slot(s, q, i), source],
                device_id={"fs": j + 1 if way == UP else j - 1},
                device_id_type=MESH,
            )
            for i, view in enumerate(views(s, q, source, g))
        ]

    def y_copies(s, q, source, side):
        return [
            pltpu.make_async_remote_copy(
                src_ref=view,
                dst_ref=view,
                send_sem=y_send.at[slot(s, q, i), source],
                recv_sem=y_recv.at[slot(s, q, i), source],
                device_id={"grp": 1 - g},
                device_id_type=MESH,
            )
            for i, view in enumerate(views(s, q, source, side))
        ]

    def start(copies):
        for copy in copies:
            copy.start()

    def wait_recv(copies):
        for copy in copies:
            copy.wait_recv()

    def wait_send(copies):
        for copy in copies:
            copy.wait_send()

    def goes_on(q, way):
        return j + 1 <= top(q) if way == UP else j - 1 >= bottom(q)

    def comes(q, source, way):
        if way == UP:
            return (source >= 0) & (j <= top(q))
        return (source < n_fs) & (j >= bottom(q))

    def own(s, way):
        for q in chunks(s):

            @pl.when(goes_on(q, way))
            def _():
                start(z_copies(s, q, j, way))

    def relay(s, last):
        for d in range(1, n_fs):
            for q in chunks(s):
                for way, source in ((UP, j - d), (DOWN, j + d)):

                    @pl.when(comes(q, source, way))
                    def _():
                        wait_recv(z_copies(s, q, source, way))

                        @pl.when(goes_on(q, way))
                        def _():
                            start(z_copies(s, q, source, way))

                        if q is None:
                            start(y_copies(s, q, source, g))
                        else:

                            @pl.when(p == q)
                            def _():
                                start(y_copies(s, q, source, g))

            if not last:

                @pl.when((j == d) & (j + 1 < n_fs))
                def _():
                    own(s + 1, UP)

                @pl.when((n_fs - 1 - j == d) & (j >= 1))
                def _():
                    own(s + 1, DOWN)

    def arrived(s):
        q = None if isinstance(s, int) and s == 0 else p
        for d in range(1, n_fs):
            wait_recv(y_copies(s, q, lax.rem(j + d, n_fs), 1 - g))

    def to_tp(src, dst, send_sem, recv_sem, to):
        return pltpu.make_async_remote_copy(
            src_ref=src,
            dst_ref=dst,
            send_sem=send_sem,
            recv_sem=recv_sem,
            device_id={"tp": to},
            device_id_type=MESH,
        )

    def tok_copy(d, source):
        return to_tp(
            tok.at[source], tok.at[source], tp_send.at[0, d], tp_recv.at[0, d], lax.rem(k + d, n_tp)
        )

    def mix_copy(d):
        to = lax.rem(k + d, n_tp)
        return to_tp(part.at[to], got.at[d], tp_send.at[1, d], tp_recv.at[1, d], to)

    def all_copies(o, at, kind):
        copies = []
        for dx in range(n_x):
            there = lax.rem(x + dx, n_x)
            if kind == "over":
                if dx:
                    view = res.at[k, at]
                    copies.append(
                        to_tp(
                            view,
                            view,
                            all_send.at[o, 0, dx],
                            all_recv.at[o, 0, dx],
                            there * 2 + c,
                        )
                    )
            else:
                back = lax.rem(x + n_x - dx, n_x) * 2
                seen = back + c if kind == "pass" else back + 1 - c
                view = res.at[seen, at]
                copies.append(
                    to_tp(view, view, all_send.at[o, 1, dx], all_recv.at[o, 1, dx], core)
                )
        return copies

    def all_begin(o, at):
        start(all_copies(o, at, "over"))
        all_copies(o, at, "pass")[0].start()

    def all_middle(o, at):
        passed = all_copies(o, at, "pass")
        for dx in range(1, n_x):
            view = res.at[lax.rem(x + n_x - dx, n_x) * 2 + c, at]
            to_tp(
                view, view, all_send.at[o, 0, dx], all_recv.at[o, 0, dx], core
            ).wait_recv()
            passed[dx].start()

    def all_end(o, at):
        wait_recv(all_copies(o, at, "take"))

    def to_pair(i, src, dst):
        return pltpu.make_async_remote_copy(
            src_ref=src,
            dst_ref=dst,
            send_sem=pair_send.at[i],
            recv_sem=pair_recv.at[i],
            device_id={"fs": pair},
            device_id_type=MESH,
        )

    barrier = pltpu.get_barrier_semaphore()
    for peer in (lax.rem(j + 1, n_fs), lax.rem(j + n_fs - 1, n_fs)):
        pl.semaphore_signal(barrier, inc=1, device_id={"fs": peer}, device_id_type=MESH)
    pl.semaphore_signal(barrier, inc=1, device_id={"grp": 1 - g}, device_id_type=MESH)
    for d in range(1, n_tp):
        pl.semaphore_signal(
            barrier, inc=1, device_id={"tp": lax.rem(k + d, n_tp)}, device_id_type=MESH
        )

    at_rows = pl.ds(pl.multiple_of(j * shard, shard), shard)
    loads = [
        pltpu.make_async_copy(ref, mix_in.at[i, at_rows, :], load_sem.at[i])
        for i, ref in enumerate((w_signal, w_outer_gate, w_inner_gate))
    ]
    loads.append(pltpu.make_async_copy(w_mix_out, mix_out.at[j], load_sem.at[3]))
    loads.append(pltpu.make_async_copy(tokens, tok.at[k], load_sem.at[4]))
    for s in range(1, stages):
        for q in (0, 1):
            cut = pl.ds(q * hidden_half + (s - 1) * LANES, LANES)
            for src, dst in (
                (w_gate.at[:, cut], ffn_in.at[s - 1, q, at_rows, pl.ds(0, LANES)]),
                (w_value.at[:, cut], ffn_in.at[s - 1, q, at_rows, pl.ds(LANES, LANES)]),
                (w_down.at[cut, :], ffn_out.at[s - 1, q, j]),
            ):
                loads.append(pltpu.make_async_copy(src, dst, load_sem.at[len(loads)]))
    start(loads)
    for copy in loads[:5]:
        copy.wait()
    pl.semaphore_wait(barrier, 3 + n_tp - 1)

    own(0, UP)
    own(0, DOWN)
    for d in range(1, n_tp):
        tok_copy(d, k).start()
    for copy in loads[5:]:
        copy.wait()

    @pl.when(j == 0)
    def _():
        for s in range(1, stages):
            own(s, UP)

    @pl.when(j == n_fs - 1)
    def _():
        for s in range(1, stages):
            own(s, DOWN)

    def norm(buffer, at, gain):
        squares = jnp.zeros((rows, 1), jnp.float32)
        for b in range(n_tp):
            values = buffer[b, at, :].astype(jnp.float32)
            squares = squares + jnp.sum(values * values, axis=-1, keepdims=True)
        scale = lax.rsqrt(squares / (n_tp * own_cols) + 1e-06)
        for b in range(n_tp):
            cut = slice(b * own_cols, (b + 1) * own_cols)
            values = buffer[b, at, :].astype(jnp.float32)
            normed[at, cut] = (values * scale * gain[:, cut]).astype(jnp.bfloat16)

    first = pl.ds(0, rows)
    for d in range(1, n_tp):
        tok_copy(d, lax.rem(k + n_tp - d, n_tp)).wait_recv()
    norm(tok, first, mix_gain)

    relay(0, False)
    arrived(0)

    def project(weight):
        product = jnp.dot(normed[first, :], weight, preferred_element_type=jnp.float32)
        return product.astype(jnp.bfloat16).astype(jnp.float32)

    gated = project(mix_in[2]) * project(mix_in[0])
    conv = conv_rows(gated, mix_taps[...], length)
    mixed = (project(mix_in[1]) * conv).astype(jnp.bfloat16)
    for b in range(n_fs):
        total[first, b * shard : (b + 1) * shard] = jnp.dot(
            mixed, mix_out[b], preferred_element_type=jnp.float32
        )
    for b in range(n_tp):
        part[b] = total[first, b * own_cols : (b + 1) * own_cols].astype(jnp.bfloat16)
    for d in range(1, n_tp):
        mix_copy(d).start()

    relay(1, False)

    mixer = part[k].astype(jnp.float32)
    for d in range(1, n_tp):
        mix_copy(d).wait_recv()
        mixer = mixer + got[d].astype(jnp.float32)
    res[k, mine, :] = (tok[k].astype(jnp.float32) + mixer).astype(jnp.bfloat16)
    swap = to_pair(0, res.at[k, mine], res.at[k, mine])
    swapped = to_pair(0, res.at[k, theirs], res.at[k, theirs])
    swap.start()
    all_begin(0, mine)

    relay(2, False)
    all_middle(0, mine)
    swapped.wait_recv()
    all_begin(1, theirs)
    all_end(0, mine)
    norm(res, mine, ffn_gain)
    relay(3, False)
    all_middle(1, theirs)
    all_end(1, theirs)
    norm(res, theirs, ffn_gain)
    total[...] = jnp.zeros_like(total)

    def feed(s):
        arrived(s)
        at = pl.multiple_of(p * hidden_half + (s - 1) * LANES, LANES)
        cut = pl.ds(at, LANES)
        both = jnp.dot(normed[...], ffn_in[s - 1, p], preferred_element_type=jnp.float32)
        both = both.astype(jnp.bfloat16).astype(jnp.float32)
        gate = conv_rows(both[:, :LANES], up_taps[0, :, cut], length) + up_bias[0:1, cut]
        value = conv_rows(both[:, LANES:], up_taps[1, :, cut], length) + up_bias[1:2, cut]
        hidden = (gate / (1.0 + jnp.exp(-gate)) * value).astype(jnp.bfloat16)
        for b in range(n_fs):
            total[:, b * shard : (b + 1) * shard] += jnp.dot(
                hidden, ffn_out[s - 1, p, b], preferred_element_type=jnp.float32
            )

    @pl.loop(1, stages)
    def _(s):
        @pl.when(s + 3 < stages - 1)
        def _():
            relay(s + 3, False)

        @pl.when(s + 3 == stages - 1)
        def _():
            relay(s + 3, True)

        feed(s)

    def core_copy(o, there, dx):
        return to_tp(
            part_ffn.at[o, there * 2 + 1 - c],
            got_core.at[o, there],
            core_send.at[o, dx],
            core_recv.at[o, dx],
            core,
        )

    def x_copy(o, dx):
        to = lax.rem(x + dx, n_x) * 2 + c
        return to_tp(sum_x.at[o, dx], got_x.at[o, dx], x_send.at[o, dx], x_recv.at[o, dx], to)

    order = [*range(1, n_x), 0]
    for o, at in enumerate((theirs, mine)):
        for b in range(n_tp):
            part_ffn[o, b] = total[at, b * own_cols : (b + 1) * own_cols].astype(jnp.bfloat16)
        for dx in order:
            core_copy(o, lax.rem(x + dx, n_x), dx).start()

    def chip_sum(o, dx):
        there = lax.rem(x + dx, n_x)
        core_copy(o, there, dx).wait_recv()
        return part_ffn[o, there * 2 + c].astype(jnp.float32) + got_core[o, there].astype(jnp.float32)

    for o in (0, 1):
        for dx in range(1, n_x):
            sum_x[o, dx] = chip_sum(o, dx).astype(jnp.bfloat16)
            x_copy(o, dx).start()

    def place_sum(o):
        value = chip_sum(o, 0)
        for dx in range(1, n_x):
            x_copy(o, dx).wait_recv()
            value = value + got_x[o, dx].astype(jnp.float32)
        return value

    sum_z[...] = place_sum(0).astype(jnp.bfloat16)
    back = to_pair(1, sum_z, got_z)
    back.start()
    value = res[k, mine, :].astype(jnp.float32) + place_sum(1)
    back.wait_recv()
    out[...] = (value + got_z[...].astype(jnp.float32)).astype(jnp.bfloat16)

    for d in range(1, n_tp):
        tok_copy(d, k).wait_send()
        mix_copy(d).wait_send()
    for o, at in enumerate((mine, theirs)):
        wait_send(all_copies(o, at, "over"))
        wait_send(all_copies(o, at, "pass"))
    for o in (0, 1):
        for dx in range(n_x):
            core_copy(o, lax.rem(x + dx, n_x), dx).wait_send()
        for dx in range(1, n_x):
            x_copy(o, dx).wait_send()
    swap.wait_send()
    back.wait_send()

    def drain(s):
        for q in chunks(s):
            for d in range(n_fs):
                for way, source in ((UP, j - d), (DOWN, j + d)):

                    @pl.when(comes(q, source, way) & goes_on(q, way))
                    def _():
                        wait_send(z_copies(s, q, source, way))

        q = None if isinstance(s, int) and s == 0 else p
        for d in range(1, n_fs):
            wait_send(y_copies(s, q, lax.rem(j + d, n_fs), g))

    drain(0)
    pl.loop(1, stages)(drain)


def fused(n_fs, n_tp, *args):
    tokens, w_signal, w_gate = args[0], args[2], args[8]
    rows, cols = tokens.shape
    shard, chans = w_signal.shape
    stages = 1 + w_gate.shape[1] // (2 * LANES)
    width = n_fs * shard
    args = list(args)
    args[1], args[7] = args[1].reshape(1, -1), args[7].reshape(1, -1)
    in_vmem = {1, 5, 7, 10, 11}
    n_x = n_tp // 2
    copies = 2 + 4 * (stages - 1)
    dma = pltpu.SemaphoreType.DMA

    def held(*shape):
        return pltpu.VMEM(shape, jnp.bfloat16)

    return pl.pallas_call(
        functools.partial(layer_kernel, n_fs, n_tp),
        out_shape=jax.ShapeDtypeStruct((rows, cols), jnp.bfloat16),
        in_specs=[
            pl.BlockSpec(memory_space=pltpu.VMEM if i in in_vmem else pl.ANY)
            for i in range(len(args))
        ],
        out_specs=pl.BlockSpec(memory_space=pltpu.VMEM),
        scratch_shapes=[
            held(3, width, chans),
            held(n_fs, chans, shard),
            held(stages - 1, 2, width, 2 * LANES),
            held(stages - 1, 2, n_fs, LANES, shard),
            held(n_tp, rows, cols),
            held(n_tp, 2 * rows, cols),
            held(2 * rows, width),
            pltpu.VMEM((2 * rows, width), jnp.float32),
            held(n_tp, rows, cols),
            held(n_tp, rows, cols),
            held(2, n_tp, rows, cols),
            held(2, n_x, rows, cols),
            held(2, n_x, rows, cols),
            held(2, n_x, rows, cols),
            held(rows, cols),
            held(rows, cols),
            dma((2, copies, n_fs)),
            dma((copies, n_fs)),
            dma((copies, n_fs)),
            dma((copies, n_fs)),
            dma((5 + 6 * (stages - 1),)),
            dma((2, n_tp)),
            dma((2, n_tp)),
            dma((2, 2, n_x)),
            dma((2, 2, n_x)),
            dma((2, n_x)),
            dma((2, n_x)),
            dma((2, n_x)),
            dma((2, n_x)),
            dma((2,)),
            dma((2,)),
        ],
        compiler_params=pltpu.CompilerParams(
            collective_id=0, has_side_effects=True, vmem_limit_bytes=62 * 1024 * 1024
        ),
    )(*args)


def solution(mesh):
    n_fs, n_tp = mesh.shape["fs"], mesh.shape["tp"]
    body = functools.partial(fused, n_fs, n_tp)
    if n_fs > 8 or n_fs % 2 or n_tp % 2 or mesh.shape["grp"] != 2:
        body = on_device
    placed = (
        P(("grp", "fs"), "tp"),
        P(),
        P("fs", "tp"),
        P("fs", "tp"),
        P("fs", "tp"),
        P(None, "tp"),
        P("tp", "fs"),
        P(),
        P("fs", "tp"),
        P("fs", "tp"),
        P(None, None, "tp"),
        P(None, "tp"),
        P("tp", "fs"),
    )
    return jax.shard_map(
        body, mesh=mesh, in_specs=placed, out_specs=P(("grp", "fs"), "tp"), check_vma=False
    )
```

```python
import functools

import jax
import jax.numpy as jnp
from jax import lax
from jax.experimental import pallas as pl
from jax.experimental.pallas import tpu as pltpu
from jax.sharding import PartitionSpec as P

SEQS_DEV = 2


def conv_positions(values, taps):
    width = values.shape[1]
    blocks = values.reshape(SEQS_DEV, -1, width)
    length = blocks.shape[1]
    padded = jnp.pad(blocks, ((0, 0), (2, 0), (0, 0)))
    result = (
        padded[:, 0:length] * taps[0]
        + padded[:, 1 : length + 1] * taps[1]
        + padded[:, 2 : length + 2] * taps[2]
    )
    return result.reshape(-1, width)


def rms_norm(stream, gain):
    values = stream.astype(jnp.float32)
    scale = lax.rsqrt(jnp.mean(values * values, axis=-1, keepdims=True) + 1e-06)
    return (values * scale * gain).astype(jnp.bfloat16)


def on_device(
    tokens,
    mix_gain,
    w_signal,
    w_outer_gate,
    w_inner_gate,
    mix_taps,
    w_mix_out,
    ffn_gain,
    w_gate,
    w_value,
    up_taps,
    up_bias,
    w_down,
):
    whole = lax.all_gather(tokens, "tp", axis=1, tiled=True)
    normed = rms_norm(whole, mix_gain)
    pieces = (
        lax.all_gather(w_signal, "fs", axis=0, tiled=True),
        lax.all_gather(w_outer_gate, "fs", axis=0, tiled=True),
        lax.all_gather(w_inner_gate, "fs", axis=0, tiled=True),
    )
    columns = normed
    signal, outer, inner = tuple(
        (jnp.dot(columns, piece, preferred_element_type=jnp.float32) for piece in pieces)
    )
    signal = signal.astype(jnp.bfloat16).astype(jnp.float32)
    outer = outer.astype(jnp.bfloat16).astype(jnp.float32)
    inner = inner.astype(jnp.bfloat16).astype(jnp.float32)
    mixed = (outer * conv_positions(inner * signal, mix_taps)).astype(jnp.bfloat16)
    mix_terms = jnp.dot(
        mixed,
        lax.all_gather(w_mix_out, "fs", axis=1, tiled=True),
        preferred_element_type=jnp.float32,
    )
    mix_sum = lax.psum_scatter(
        mix_terms.astype(jnp.bfloat16), "tp", scatter_dimension=1, tiled=True
    ).astype(jnp.float32)
    resid = (tokens.astype(jnp.float32) + mix_sum).astype(jnp.bfloat16)
    whole_ffn = lax.all_gather(resid, "tp", axis=1, tiled=True)
    normed_ffn = rms_norm(whole_ffn, ffn_gain)
    pieces = (
        lax.all_gather(w_gate, "fs", axis=0, tiled=True),
        lax.all_gather(w_value, "fs", axis=0, tiled=True),
    )
    columns = normed_ffn
    gate = jnp.dot(columns, pieces[0], preferred_element_type=jnp.float32)
    value = jnp.dot(columns, pieces[1], preferred_element_type=jnp.float32)
    gate = gate.astype(jnp.bfloat16).astype(jnp.float32)
    value = value.astype(jnp.bfloat16).astype(jnp.float32)
    gate_conv = conv_positions(gate, up_taps[0]) + up_bias[0]
    value_conv = conv_positions(value, up_taps[1]) + up_bias[1]
    hidden = (jax.nn.silu(gate_conv) * value_conv).astype(jnp.bfloat16)
    ffn_terms = jnp.dot(
        hidden, lax.all_gather(w_down, "fs", axis=1, tiled=True), preferred_element_type=jnp.float32
    )
    ffn_sum = lax.psum_scatter(
        ffn_terms.astype(jnp.bfloat16), "tp", scatter_dimension=1, tiled=True
    ).astype(jnp.float32)
    return (resid.astype(jnp.float32) + ffn_sum).astype(jnp.bfloat16)


MESH = pl.DeviceIdType.MESH
UP, DOWN = 0, 1
LANES = 128


def shifted(values, by, length):
    rolled = pltpu.roll(values, by, 0)
    position = lax.rem(lax.broadcasted_iota(jnp.int32, values.shape, 0), length)
    return jnp.where(position < by, 0.0, rolled)


def conv_rows(values, taps, length):
    return (
        shifted(values, 2, length) * taps[0:1]
        + shifted(values, 1, length) * taps[1:2]
        + values * taps[2:3]
    )


def layer_kernel(
    n_fs,
    n_tp,
    tokens,
    mix_gain,
    w_signal,
    w_outer_gate,
    w_inner_gate,
    mix_taps,
    w_mix_out,
    ffn_gain,
    w_gate,
    w_value,
    up_taps,
    up_bias,
    w_down,
    out,
    mix_in,
    mix_out,
    ffn_in,
    ffn_out,
    tok,
    res,
    normed,
    hidden,
    part,
    got,
    part_ffn,
    got_core,
    sum_x,
    got_x,
    sum_z,
    got_z,
    z_send,
    z_recv,
    y_send,
    y_recv,
    load_sem,
    tp_send,
    tp_recv,
    all_send,
    all_recv,
    core_send,
    core_recv,
    x_send,
    x_recv,
    pair_send,
    pair_recv,
):
    g, j, k = lax.axis_index("grp"), lax.axis_index("fs"), lax.axis_index("tp")
    rows, own_cols = tokens.shape
    length = rows // SEQS_DEV
    shard, chans = w_signal.shape
    half = shard // 2
    hidden_half = w_gate.shape[1] // 2
    n_in, n_out = hidden_half // LANES, shard // LANES
    n_x = n_tp // 2
    x, c = k // 2, lax.rem(k, 2)
    core = k + 1 - 2 * c
    p = lax.rem(j, 2)
    pair = j + 1 - 2 * p
    mine = pl.ds(pl.multiple_of(p * rows, rows), rows)
    theirs = pl.ds(pl.multiple_of((1 - p) * rows, rows), rows)

    mix = ("mix", 0)
    order = [mix, *(("in", t) for t in range(n_in)), *(("out", u) for u in range(n_out))]

    def chunks(stage):
        return (None,) if stage[0] == "mix" else (0, 1)

    def top(q):
        return n_fs - 1 if q is None or (n_fs - 1) % 2 == q else n_fs - 2

    def bottom(q):
        return 0 if q is None else q

    def views(stage, q, source, side):
        kind, i = stage
        at_rows = pl.ds(pl.multiple_of((source * 2 + side) * half, half), half)
        tall = (chans if kind == "mix" else hidden_half) // 2
        at_chans = pl.ds(pl.multiple_of(side * tall, tall), tall)
        if kind == "mix":
            return mix_in.at[:, at_rows, :], mix_out.at[source, at_chans, :]
        if kind == "in":
            return (ffn_in.at[i, q, at_rows, :],)
        lanes = pl.ds(pl.multiple_of(source * LANES, LANES), LANES)
        return (ffn_out.at[i, q, at_chans, lanes],)

    def slot(stage, q, i):
        kind, at = stage
        if kind == "mix":
            return i
        return 2 + 2 * (at if kind == "in" else at + n_in) + q

    def z_copies(s, q, source, way):
        return [
            pltpu.make_async_remote_copy(
                src_ref=view,
                dst_ref=view,
                send_sem=z_send.at[way, slot(s, q, i), source],
                recv_sem=z_recv.at[slot(s, q, i), source],
                device_id={"fs": j + 1 if way == UP else j - 1},
                device_id_type=MESH,
            )
            for i, view in enumerate(views(s, q, source, g))
        ]

    def y_copies(s, q, source, side):
        return [
            pltpu.make_async_remote_copy(
                src_ref=view,
                dst_ref=view,
                send_sem=y_send.at[slot(s, q, i), source],
                recv_sem=y_recv.at[slot(s, q, i), source],
                device_id={"grp": 1 - g},
                device_id_type=MESH,
            )
            for i, view in enumerate(views(s, q, source, side))
        ]

    def start(copies):
        for copy in copies:
            copy.start()

    def wait_recv(copies):
        for copy in copies:
            copy.wait_recv()

    def wait_send(copies):
        for copy in copies:
            copy.wait_send()

    def goes_on(q, way):
        return j + 1 <= top(q) if way == UP else j - 1 >= bottom(q)

    def comes(q, source, way):
        if way == UP:
            return (source >= 0) & (j <= top(q))
        return (source < n_fs) & (j >= bottom(q))

    def own(s, way):
        for q in chunks(s):

            @pl.when(goes_on(q, way))
            def _():
                start(z_copies(s, q, j, way))

    def relay(s):
        at = order.index(s)
        following = order[at + 1] if at + 1 < len(order) else None
        for d in range(1, n_fs):
            for q in chunks(s):
                for way, source in ((UP, j - d), (DOWN, j + d)):

                    @pl.when(comes(q, source, way))
                    def _():
                        wait_recv(z_copies(s, q, source, way))

                        @pl.when(goes_on(q, way))
                        def _():
                            start(z_copies(s, q, source, way))

                        if q is None:
                            start(y_copies(s, q, source, g))
                        else:

                            @pl.when(p == q)
                            def _():
                                start(y_copies(s, q, source, g))

            if following:

                @pl.when((j == d) & (j + 1 < n_fs))
                def _():
                    own(following, UP)

                @pl.when((n_fs - 1 - j == d) & (j >= 1))
                def _():
                    own(following, DOWN)

    def arrived(s):
        q = None if s[0] == "mix" else p
        for d in range(1, n_fs):
            wait_recv(y_copies(s, q, lax.rem(j + d, n_fs), 1 - g))

    def to_tp(src, dst, send_sem, recv_sem, to):
        return pltpu.make_async_remote_copy(
            src_ref=src,
            dst_ref=dst,
            send_sem=send_sem,
            recv_sem=recv_sem,
            device_id={"tp": to},
            device_id_type=MESH,
        )

    def tok_copy(d, source):
        return to_tp(
            tok.at[source], tok.at[source], tp_send.at[0, d], tp_recv.at[0, d], lax.rem(k + d, n_tp)
        )

    def mix_copy(d):
        to = lax.rem(k + d, n_tp)
        return to_tp(part.at[to], got.at[d], tp_send.at[1, d], tp_recv.at[1, d], to)

    def all_copies(o, at, kind):
        copies = []
        for dx in range(n_x):
            there = lax.rem(x + dx, n_x)
            if kind == "over":
                if dx:
                    view = res.at[k, at]
                    copies.append(
                        to_tp(
                            view,
                            view,
                            all_send.at[o, 0, dx],
                            all_recv.at[o, 0, dx],
                            there * 2 + c,
                        )
                    )
            else:
                back = lax.rem(x + n_x - dx, n_x) * 2
                seen = back + c if kind == "pass" else back + 1 - c
                view = res.at[seen, at]
                copies.append(
                    to_tp(view, view, all_send.at[o, 1, dx], all_recv.at[o, 1, dx], core)
                )
        return copies

    def all_begin(o, at):
        start(all_copies(o, at, "over"))
        all_copies(o, at, "pass")[0].start()

    def all_middle(o, at):
        passed = all_copies(o, at, "pass")
        for dx in range(1, n_x):
            view = res.at[lax.rem(x + n_x - dx, n_x) * 2 + c, at]
            to_tp(
                view, view, all_send.at[o, 0, dx], all_recv.at[o, 0, dx], core
            ).wait_recv()
            passed[dx].start()

    def all_end(o, at):
        wait_recv(all_copies(o, at, "take"))

    def to_pair(i, src, dst):
        return pltpu.make_async_remote_copy(
            src_ref=src,
            dst_ref=dst,
            send_sem=pair_send.at[i],
            recv_sem=pair_recv.at[i],
            device_id={"fs": pair},
            device_id_type=MESH,
        )

    barrier = pltpu.get_barrier_semaphore()
    for peer in (lax.rem(j + 1, n_fs), lax.rem(j + n_fs - 1, n_fs)):
        pl.semaphore_signal(barrier, inc=1, device_id={"fs": peer}, device_id_type=MESH)
    pl.semaphore_signal(barrier, inc=1, device_id={"grp": 1 - g}, device_id_type=MESH)
    for d in range(1, n_tp):
        pl.semaphore_signal(
            barrier, inc=1, device_id={"tp": lax.rem(k + d, n_tp)}, device_id_type=MESH
        )

    at_rows = pl.ds(pl.multiple_of(j * shard, shard), shard)
    loads = [
        pltpu.make_async_copy(ref, mix_in.at[i, at_rows, :], load_sem.at[i])
        for i, ref in enumerate((w_signal, w_outer_gate, w_inner_gate))
    ]
    loads.append(pltpu.make_async_copy(w_mix_out, mix_out.at[j], load_sem.at[3]))
    loads.append(pltpu.make_async_copy(tokens, tok.at[k], load_sem.at[4]))
    for q in (0, 1):
        for t in range(n_in):
            at = pl.ds(q * hidden_half + t * LANES, LANES)
            for i, ref in enumerate((w_gate, w_value)):
                dst = ffn_in.at[t, q, at_rows, pl.ds(i * LANES, LANES)]
                loads.append(pltpu.make_async_copy(ref.at[:, at], dst, load_sem.at[len(loads)]))
        for u in range(n_out):
            src = w_down.at[pl.ds(q * hidden_half, hidden_half), pl.ds(u * LANES, LANES)]
            lanes = pl.ds(pl.multiple_of(j * LANES, LANES), LANES)
            dst = ffn_out.at[u, q, :, lanes]
            loads.append(pltpu.make_async_copy(src, dst, load_sem.at[len(loads)]))
    start(loads)
    for copy in loads[:5]:
        copy.wait()
    pl.semaphore_wait(barrier, 3 + n_tp - 1)

    own(mix, UP)
    own(mix, DOWN)
    for d in range(1, n_tp):
        tok_copy(d, k).start()
    for copy in loads[5:]:
        copy.wait()

    @pl.when(j == 0)
    def _():
        for s in order[1:]:
            own(s, UP)

    @pl.when(j == n_fs - 1)
    def _():
        for s in order[1:]:
            own(s, DOWN)

    def norm(buffer, at, gain):
        squares = jnp.zeros((rows, 1), jnp.float32)
        for b in range(n_tp):
            values = buffer[b, at, :].astype(jnp.float32)
            squares = squares + jnp.sum(values * values, axis=-1, keepdims=True)
        scale = lax.rsqrt(squares / (n_tp * own_cols) + 1e-06)
        for b in range(n_tp):
            cut = slice(b * own_cols, (b + 1) * own_cols)
            values = buffer[b, at, :].astype(jnp.float32)
            normed[at, cut] = (values * scale * gain[:, cut]).astype(jnp.bfloat16)

    first = pl.ds(0, rows)
    for d in range(1, n_tp):
        tok_copy(d, lax.rem(k + n_tp - d, n_tp)).wait_recv()
    norm(tok, first, mix_gain)

    relay(mix)
    arrived(mix)

    def project(weight):
        product = jnp.dot(normed[first, :], weight, preferred_element_type=jnp.float32)
        return product.astype(jnp.bfloat16).astype(jnp.float32)

    gated = project(mix_in[2]) * project(mix_in[0])
    conv = conv_rows(gated, mix_taps[...], length)
    mixed = (project(mix_in[1]) * conv).astype(jnp.bfloat16)
    for b in range(n_fs):
        part[b] = jnp.dot(mixed, mix_out[b], preferred_element_type=jnp.float32).astype(jnp.bfloat16)
    for d in range(1, n_tp):
        mix_copy(d).start()

    relay(order[1])

    mixer = part[k].astype(jnp.float32)
    for d in range(1, n_tp):
        mix_copy(d).wait_recv()
        mixer = mixer + got[d].astype(jnp.float32)
    res[k, mine, :] = (tok[k].astype(jnp.float32) + mixer).astype(jnp.bfloat16)
    swap = to_pair(0, res.at[k, mine], res.at[k, mine])
    swapped = to_pair(0, res.at[k, theirs], res.at[k, theirs])
    swap.start()
    all_begin(0, mine)

    relay(order[2])
    all_middle(0, mine)
    swapped.wait_recv()
    all_begin(1, theirs)
    all_end(0, mine)
    norm(res, mine, ffn_gain)
    relay(order[3])
    all_middle(1, theirs)
    all_end(1, theirs)
    norm(res, theirs, ffn_gain)
    relay(order[4])

    def feed(t):
        arrived(("in", t))
        cut = pl.ds(pl.multiple_of(p * hidden_half + t * LANES, LANES), LANES)
        both = jnp.dot(normed[...], ffn_in[t, p], preferred_element_type=jnp.float32)
        both = both.astype(jnp.bfloat16).astype(jnp.float32)
        gate = conv_rows(both[:, :LANES], up_taps[0, :, cut], length) + up_bias[0:1, cut]
        value = conv_rows(both[:, LANES:], up_taps[1, :, cut], length) + up_bias[1:2, cut]
        units = (gate / (1.0 + jnp.exp(-gate)) * value).astype(jnp.bfloat16)
        hidden[:, pl.ds(pl.multiple_of(t * LANES, LANES), LANES)] = units

    beside = {0: 5, 1: 6, 3: 7}

    @pl.loop(0, n_in)
    def _(t):
        for at, index in beside.items():

            @pl.when(t == at)
            def _():
                relay(order[index])

        feed(t)

    def core_copy(u, dx):
        there = lax.rem(x + dx, n_x)
        return to_tp(
            part_ffn.at[u, :, there * 2 + 1 - c],
            got_core.at[u, :, there],
            core_send.at[u, dx],
            core_recv.at[u, dx],
            core,
        )

    def x_copy(u, dx):
        to = lax.rem(x + dx, n_x) * 2 + c
        return to_tp(sum_x.at[u, dx], got_x.at[u, dx], x_send.at[u, dx], x_recv.at[u, dx], to)

    def back(u):
        return to_pair(1 + u, sum_z.at[u], got_z.at[u])

    def chip_sum(u, o, dx):
        there = lax.rem(x + dx, n_x)
        mine_there = part_ffn[u, o, there * 2 + c].astype(jnp.float32)
        return mine_there + got_core[u, o, there].astype(jnp.float32)

    def place_sum(u, o):
        value = chip_sum(u, o, 0)
        for dx in range(1, n_x):
            value = value + got_x[u, dx, o].astype(jnp.float32)
        return value

    def down(u):
        arrived(("out", u))
        for o, at in enumerate((theirs, mine)):
            terms = jnp.dot(hidden[at, :], ffn_out[u, p], preferred_element_type=jnp.float32)
            for b in range(n_tp):
                part_ffn[u, o, b] = terms[:, b * LANES : (b + 1) * LANES].astype(jnp.bfloat16)
        for dx in (*range(1, n_x), 0):
            core_copy(u, dx).start()

    def over_x(u):
        for dx in range(1, n_x):
            core_copy(u, dx).wait_recv()
            for o in (0, 1):
                sum_x[u, dx, o] = chip_sum(u, o, dx).astype(jnp.bfloat16)
            x_copy(u, dx).start()

    def over_z(u):
        core_copy(u, 0).wait_recv()
        for dx in range(1, n_x):
            x_copy(u, dx).wait_recv()
        sum_z[u] = place_sum(u, 0).astype(jnp.bfloat16)
        back(u).start()

    for u in range(n_out):
        if 8 + u < len(order):
            relay(order[8 + u])
        down(u)
        if u >= 1:
            over_x(u - 1)
        if u >= 2:
            over_z(u - 2)
    over_x(n_out - 1)
    for u in range(max(n_out - 2, 0), n_out):
        over_z(u)
    for u in range(n_out):
        cut = slice(u * LANES, (u + 1) * LANES)
        value = res[k, mine, cut].astype(jnp.float32) + place_sum(u, 1)
        back(u).wait_recv()
        out[:, cut] = (value + got_z[u].astype(jnp.float32)).astype(jnp.bfloat16)

    for d in range(1, n_tp):
        tok_copy(d, k).wait_send()
        mix_copy(d).wait_send()
    for o, at in enumerate((mine, theirs)):
        wait_send(all_copies(o, at, "over"))
        wait_send(all_copies(o, at, "pass"))
    for u in range(n_out):
        for dx in range(n_x):
            core_copy(u, dx).wait_send()
        for dx in range(1, n_x):
            x_copy(u, dx).wait_send()
        back(u).wait_send()
    swap.wait_send()

    def drain(s):
        for q in chunks(s):
            for d in range(n_fs):
                for way, source in ((UP, j - d), (DOWN, j + d)):

                    @pl.when(comes(q, source, way) & goes_on(q, way))
                    def _():
                        wait_send(z_copies(s, q, source, way))

        q = None if s[0] == "mix" else p
        for d in range(1, n_fs):
            wait_send(y_copies(s, q, lax.rem(j + d, n_fs), g))

    drain(mix)

    @pl.loop(0, n_in)
    def _(t):
        drain(("in", t))

    @pl.loop(0, n_out)
    def _(u):
        drain(("out", u))


def fused(n_fs, n_tp, *args):
    tokens, w_signal, w_gate = args[0], args[2], args[8]
    rows, cols = tokens.shape
    shard, chans = w_signal.shape
    hidden = w_gate.shape[1] // 2
    n_in, n_out = hidden // LANES, shard // LANES
    width = n_fs * shard
    args = list(args)
    args[1], args[7] = args[1].reshape(1, -1), args[7].reshape(1, -1)
    in_vmem = {1, 5, 7, 10, 11}
    n_x = n_tp // 2
    copies = 2 + 2 * (n_in + n_out)
    dma = pltpu.SemaphoreType.DMA

    def held(*shape):
        return pltpu.VMEM(shape, jnp.bfloat16)

    return pl.pallas_call(
        functools.partial(layer_kernel, n_fs, n_tp),
        out_shape=jax.ShapeDtypeStruct((rows, cols), jnp.bfloat16),
        in_specs=[
            pl.BlockSpec(memory_space=pltpu.VMEM if i in in_vmem else pl.ANY)
            for i in range(len(args))
        ],
        out_specs=pl.BlockSpec(memory_space=pltpu.VMEM),
        scratch_shapes=[
            held(3, width, chans),
            held(n_fs, chans, shard),
            held(n_in, 2, width, 2 * LANES),
            held(n_out, 2, hidden, n_fs * LANES),
            held(n_tp, rows, cols),
            held(n_tp, 2 * rows, cols),
            held(2 * rows, width),
            held(2 * rows, hidden),
            held(n_tp, rows, cols),
            held(n_tp, rows, cols),
            held(n_out, 2, n_tp, rows, LANES),
            held(n_out, 2, n_x, rows, LANES),
            held(n_out, n_x, 2, rows, LANES),
            held(n_out, n_x, 2, rows, LANES),
            held(n_out, rows, LANES),
            held(n_out, rows, LANES),
            dma((2, copies, n_fs)),
            dma((copies, n_fs)),
            dma((copies, n_fs)),
            dma((copies, n_fs)),
            dma((5 + 4 * n_in + 2 * n_out,)),
            dma((2, n_tp)),
            dma((2, n_tp)),
            dma((2, 2, n_x)),
            dma((2, 2, n_x)),
            dma((n_out, n_x)),
            dma((n_out, n_x)),
            dma((n_out, n_x)),
            dma((n_out, n_x)),
            dma((1 + n_out,)),
            dma((1 + n_out,)),
        ],
        compiler_params=pltpu.CompilerParams(
            collective_id=0, has_side_effects=True, vmem_limit_bytes=62 * 1024 * 1024
        ),
    )(*args)


def solution(mesh):
    n_fs, n_tp = mesh.shape["fs"], mesh.shape["tp"]
    body = functools.partial(fused, n_fs, n_tp)
    if n_fs > 8 or n_fs != n_tp or n_fs % 2 or mesh.shape["grp"] != 2:
        body = on_device
    placed = (
        P(("grp", "fs"), "tp"),
        P(),
        P("fs", "tp"),
        P("fs", "tp"),
        P("fs", "tp"),
        P(None, "tp"),
        P("tp", "fs"),
        P(),
        P("fs", "tp"),
        P("fs", "tp"),
        P(None, None, "tp"),
        P(None, "tp"),
        P("tp", "fs"),
    )
    return jax.shard_map(
        body, mesh=mesh, in_specs=placed, out_specs=P(("grp", "fs"), "tp"), check_vma=False
    )
```

```python
import functools

import jax
import jax.numpy as jnp
from jax import lax
from jax.experimental import pallas as pl
from jax.experimental.pallas import tpu as pltpu
from jax.sharding import PartitionSpec as P

SEQS_DEV = 2


def conv_positions(values, taps):
    width = values.shape[1]
    blocks = values.reshape(SEQS_DEV, -1, width)
    length = blocks.shape[1]
    padded = jnp.pad(blocks, ((0, 0), (2, 0), (0, 0)))
    result = (
        padded[:, 0:length] * taps[0]
        + padded[:, 1 : length + 1] * taps[1]
        + padded[:, 2 : length + 2] * taps[2]
    )
    return result.reshape(-1, width)


def rms_norm(stream, gain):
    values = stream.astype(jnp.float32)
    scale = lax.rsqrt(jnp.mean(values * values, axis=-1, keepdims=True) + 1e-06)
    return (values * scale * gain).astype(jnp.bfloat16)


def on_device(
    tokens,
    mix_gain,
    w_signal,
    w_outer_gate,
    w_inner_gate,
    mix_taps,
    w_mix_out,
    ffn_gain,
    w_gate,
    w_value,
    up_taps,
    up_bias,
    w_down,
):
    whole = lax.all_gather(tokens, "tp", axis=1, tiled=True)
    normed = rms_norm(whole, mix_gain)
    pieces = (
        lax.all_gather(w_signal, "fs", axis=0, tiled=True),
        lax.all_gather(w_outer_gate, "fs", axis=0, tiled=True),
        lax.all_gather(w_inner_gate, "fs", axis=0, tiled=True),
    )
    columns = normed
    signal, outer, inner = tuple(
        (jnp.dot(columns, piece, preferred_element_type=jnp.float32) for piece in pieces)
    )
    signal = signal.astype(jnp.bfloat16).astype(jnp.float32)
    outer = outer.astype(jnp.bfloat16).astype(jnp.float32)
    inner = inner.astype(jnp.bfloat16).astype(jnp.float32)
    mixed = (outer * conv_positions(inner * signal, mix_taps)).astype(jnp.bfloat16)
    mix_terms = jnp.dot(
        mixed,
        lax.all_gather(w_mix_out, "fs", axis=1, tiled=True),
        preferred_element_type=jnp.float32,
    )
    mix_sum = lax.psum_scatter(
        mix_terms.astype(jnp.bfloat16), "tp", scatter_dimension=1, tiled=True
    ).astype(jnp.float32)
    resid = (tokens.astype(jnp.float32) + mix_sum).astype(jnp.bfloat16)
    whole_ffn = lax.all_gather(resid, "tp", axis=1, tiled=True)
    normed_ffn = rms_norm(whole_ffn, ffn_gain)
    pieces = (
        lax.all_gather(w_gate, "fs", axis=0, tiled=True),
        lax.all_gather(w_value, "fs", axis=0, tiled=True),
    )
    columns = normed_ffn
    gate = jnp.dot(columns, pieces[0], preferred_element_type=jnp.float32)
    value = jnp.dot(columns, pieces[1], preferred_element_type=jnp.float32)
    gate = gate.astype(jnp.bfloat16).astype(jnp.float32)
    value = value.astype(jnp.bfloat16).astype(jnp.float32)
    gate_conv = conv_positions(gate, up_taps[0]) + up_bias[0]
    value_conv = conv_positions(value, up_taps[1]) + up_bias[1]
    hidden = (jax.nn.silu(gate_conv) * value_conv).astype(jnp.bfloat16)
    ffn_terms = jnp.dot(
        hidden, lax.all_gather(w_down, "fs", axis=1, tiled=True), preferred_element_type=jnp.float32
    )
    ffn_sum = lax.psum_scatter(
        ffn_terms.astype(jnp.bfloat16), "tp", scatter_dimension=1, tiled=True
    ).astype(jnp.float32)
    return (resid.astype(jnp.float32) + ffn_sum).astype(jnp.bfloat16)


MESH = pl.DeviceIdType.MESH
UP, DOWN = 0, 1
LANES = 128


def shifted(values, by, length):
    rolled = pltpu.roll(values, by, 0)
    position = lax.rem(lax.broadcasted_iota(jnp.int32, values.shape, 0), length)
    return jnp.where(position < by, 0.0, rolled)


def conv_rows(values, taps, length):
    return (
        shifted(values, 2, length) * taps[0:1]
        + shifted(values, 1, length) * taps[1:2]
        + values * taps[2:3]
    )


def layer_kernel(
    n_fs,
    n_tp,
    tokens,
    mix_gain,
    w_signal,
    w_outer_gate,
    w_inner_gate,
    mix_taps,
    w_mix_out,
    ffn_gain,
    w_gate,
    w_value,
    up_taps,
    up_bias,
    w_down,
    out,
    mix_in,
    mix_out,
    ffn_in,
    ffn_out,
    tok,
    res,
    normed,
    hidden,
    part,
    got,
    part_ffn,
    got_core,
    sum_x,
    got_x,
    sum_z,
    got_z,
    z_send,
    z_recv,
    y_send,
    y_recv,
    load_sem,
    tp_send,
    tp_recv,
    all_send,
    all_recv,
    core_send,
    core_recv,
    x_send,
    x_recv,
    pair_send,
    pair_recv,
):
    g, j, k = lax.axis_index("grp"), lax.axis_index("fs"), lax.axis_index("tp")
    rows, own_cols = tokens.shape
    length = rows // SEQS_DEV
    shard, chans = w_signal.shape
    half = shard // 2
    hidden_half = w_gate.shape[1] // 2
    n_in, n_out = hidden_half // LANES, shard // LANES
    n_x = n_tp // 2
    x, c = k // 2, lax.rem(k, 2)
    core = k + 1 - 2 * c
    p = lax.rem(j, 2)
    pair = j + 1 - 2 * p
    mine = pl.ds(pl.multiple_of(p * rows, rows), rows)
    theirs = pl.ds(pl.multiple_of((1 - p) * rows, rows), rows)

    mix = ("mix", 0)
    order = [mix, *(("in", t) for t in range(n_in)), *(("out", u) for u in range(n_out))]

    def chunks(stage):
        return (None,) if stage[0] == "mix" else (0, 1)

    def top(q):
        return n_fs - 1 if q is None or (n_fs - 1) % 2 == q else n_fs - 2

    def bottom(q):
        return 0 if q is None else q

    def views(stage, q, source, side):
        kind, i = stage
        at_rows = pl.ds(pl.multiple_of((source * 2 + side) * half, half), half)
        tall = (chans if kind == "mix" else hidden_half) // 2
        at_chans = pl.ds(pl.multiple_of(side * tall, tall), tall)
        if kind == "mix":
            return mix_in.at[:, at_rows, :], mix_out.at[source, at_chans, :]
        if kind == "in":
            return (ffn_in.at[i, q, at_rows, :],)
        lanes = pl.ds(pl.multiple_of(source * LANES, LANES), LANES)
        return (ffn_out.at[i, q, at_chans, lanes],)

    def slot(stage, q, i):
        kind, at = stage
        if kind == "mix":
            return i
        return 2 + 2 * (at if kind == "in" else at + n_in) + q

    def z_copies(s, q, source, way):
        return [
            pltpu.make_async_remote_copy(
                src_ref=view,
                dst_ref=view,
                send_sem=z_send.at[way, slot(s, q, i), source],
                recv_sem=z_recv.at[slot(s, q, i), source],
                device_id={"fs": j + 1 if way == UP else j - 1},
                device_id_type=MESH,
            )
            for i, view in enumerate(views(s, q, source, g))
        ]

    def y_copies(s, q, source, side):
        return [
            pltpu.make_async_remote_copy(
                src_ref=view,
                dst_ref=view,
                send_sem=y_send.at[slot(s, q, i), source],
                recv_sem=y_recv.at[slot(s, q, i), source],
                device_id={"grp": 1 - g},
                device_id_type=MESH,
            )
            for i, view in enumerate(views(s, q, source, side))
        ]

    def start(copies):
        for copy in copies:
            copy.start()

    def wait_recv(copies):
        for copy in copies:
            copy.wait_recv()

    def wait_send(copies):
        for copy in copies:
            copy.wait_send()

    def goes_on(q, way):
        return j + 1 <= top(q) if way == UP else j - 1 >= bottom(q)

    def comes(q, source, way):
        if way == UP:
            return (source >= 0) & (j <= top(q))
        return (source < n_fs) & (j >= bottom(q))

    def own(s, way):
        for q in chunks(s):

            @pl.when(goes_on(q, way))
            def _():
                start(z_copies(s, q, j, way))

    def relay(s):
        at = order.index(s)
        following = order[at + 2 : at + 3] if at else order[1:3]
        for d in range(1, n_fs):
            for q in chunks(s):
                for way, source in ((UP, j - d), (DOWN, j + d)):

                    @pl.when(comes(q, source, way))
                    def _():
                        wait_recv(z_copies(s, q, source, way))

                        @pl.when(goes_on(q, way))
                        def _():
                            start(z_copies(s, q, source, way))

                        if q is None:
                            start(y_copies(s, q, source, g))
                        else:

                            @pl.when(p == q)
                            def _():
                                start(y_copies(s, q, source, g))

            if following:

                @pl.when((j == d) & (j + 1 < n_fs))
                def _():
                    for later in following:
                        own(later, UP)

                @pl.when((n_fs - 1 - j == d) & (j >= 1))
                def _():
                    for later in following:
                        own(later, DOWN)

    def arrived(s):
        q = None if s[0] == "mix" else p
        for d in range(1, n_fs):
            wait_recv(y_copies(s, q, lax.rem(j + d, n_fs), 1 - g))

    def to_tp(src, dst, send_sem, recv_sem, to):
        return pltpu.make_async_remote_copy(
            src_ref=src,
            dst_ref=dst,
            send_sem=send_sem,
            recv_sem=recv_sem,
            device_id={"tp": to},
            device_id_type=MESH,
        )

    def tok_copy(d, source):
        return to_tp(
            tok.at[source], tok.at[source], tp_send.at[0, d], tp_recv.at[0, d], lax.rem(k + d, n_tp)
        )

    def mix_copy(d):
        to = lax.rem(k + d, n_tp)
        return to_tp(part.at[to], got.at[d], tp_send.at[1, d], tp_recv.at[1, d], to)

    def all_copies(o, at, kind):
        copies = []
        for dx in range(n_x):
            there = lax.rem(x + dx, n_x)
            if kind == "over":
                if dx:
                    view = res.at[k, at]
                    copies.append(
                        to_tp(
                            view,
                            view,
                            all_send.at[o, 0, dx],
                            all_recv.at[o, 0, dx],
                            there * 2 + c,
                        )
                    )
            else:
                back = lax.rem(x + n_x - dx, n_x) * 2
                seen = back + c if kind == "pass" else back + 1 - c
                view = res.at[seen, at]
                copies.append(
                    to_tp(view, view, all_send.at[o, 1, dx], all_recv.at[o, 1, dx], core)
                )
        return copies

    def all_begin(o, at):
        start(all_copies(o, at, "over"))
        all_copies(o, at, "pass")[0].start()

    def all_middle(o, at):
        passed = all_copies(o, at, "pass")
        for dx in range(1, n_x):
            view = res.at[lax.rem(x + n_x - dx, n_x) * 2 + c, at]
            to_tp(
                view, view, all_send.at[o, 0, dx], all_recv.at[o, 0, dx], core
            ).wait_recv()
            passed[dx].start()

    def all_end(o, at):
        wait_recv(all_copies(o, at, "take"))

    def to_pair(i, src, dst):
        return pltpu.make_async_remote_copy(
            src_ref=src,
            dst_ref=dst,
            send_sem=pair_send.at[i],
            recv_sem=pair_recv.at[i],
            device_id={"fs": pair},
            device_id_type=MESH,
        )

    barrier = pltpu.get_barrier_semaphore()
    for peer in (lax.rem(j + 1, n_fs), lax.rem(j + n_fs - 1, n_fs)):
        pl.semaphore_signal(barrier, inc=1, device_id={"fs": peer}, device_id_type=MESH)
    pl.semaphore_signal(barrier, inc=1, device_id={"grp": 1 - g}, device_id_type=MESH)
    for d in range(1, n_tp):
        pl.semaphore_signal(
            barrier, inc=1, device_id={"tp": lax.rem(k + d, n_tp)}, device_id_type=MESH
        )

    at_rows = pl.ds(pl.multiple_of(j * shard, shard), shard)
    loads = [
        pltpu.make_async_copy(ref, mix_in.at[i, at_rows, :], load_sem.at[i])
        for i, ref in enumerate((w_signal, w_outer_gate, w_inner_gate))
    ]
    loads.append(pltpu.make_async_copy(w_mix_out, mix_out.at[j], load_sem.at[3]))
    loads.append(pltpu.make_async_copy(tokens, tok.at[k], load_sem.at[4]))
    for q in (0, 1):
        for t in range(n_in):
            at = pl.ds(q * hidden_half + t * LANES, LANES)
            for i, ref in enumerate((w_gate, w_value)):
                dst = ffn_in.at[t, q, at_rows, pl.ds(i * LANES, LANES)]
                loads.append(pltpu.make_async_copy(ref.at[:, at], dst, load_sem.at[len(loads)]))
        for u in range(n_out):
            src = w_down.at[pl.ds(q * hidden_half, hidden_half), pl.ds(u * LANES, LANES)]
            lanes = pl.ds(pl.multiple_of(j * LANES, LANES), LANES)
            dst = ffn_out.at[u, q, :, lanes]
            loads.append(pltpu.make_async_copy(src, dst, load_sem.at[len(loads)]))
    start(loads)
    for copy in loads[:5]:
        copy.wait()
    pl.semaphore_wait(barrier, 3 + n_tp - 1)

    own(mix, UP)
    own(mix, DOWN)
    for d in range(1, n_tp):
        tok_copy(d, k).start()
    for copy in loads[5:]:
        copy.wait()

    @pl.when(j == 0)
    def _():
        for s in order[1:]:
            own(s, UP)

    @pl.when(j == n_fs - 1)
    def _():
        for s in order[1:]:
            own(s, DOWN)

    def norm(buffer, at, gain):
        squares = jnp.zeros((rows, 1), jnp.float32)
        for b in range(n_tp):
            values = buffer[b, at, :].astype(jnp.float32)
            squares = squares + jnp.sum(values * values, axis=-1, keepdims=True)
        scale = lax.rsqrt(squares / (n_tp * own_cols) + 1e-06)
        for b in range(n_tp):
            cut = slice(b * own_cols, (b + 1) * own_cols)
            values = buffer[b, at, :].astype(jnp.float32)
            normed[at, cut] = (values * scale * gain[:, cut]).astype(jnp.bfloat16)

    first = pl.ds(0, rows)
    for d in range(1, n_tp):
        tok_copy(d, lax.rem(k + n_tp - d, n_tp)).wait_recv()
    norm(tok, first, mix_gain)

    relay(mix)
    relay(order[1])
    arrived(mix)

    def project(weight):
        product = jnp.dot(normed[first, :], weight, preferred_element_type=jnp.float32)
        return product.astype(jnp.bfloat16).astype(jnp.float32)

    gated = project(mix_in[2]) * project(mix_in[0])
    conv = conv_rows(gated, mix_taps[...], length)
    mixed = (project(mix_in[1]) * conv).astype(jnp.bfloat16)
    for b in range(n_fs):
        part[b] = jnp.dot(mixed, mix_out[b], preferred_element_type=jnp.float32).astype(jnp.bfloat16)
    for d in range(1, n_tp):
        mix_copy(d).start()


    mixer = part[k].astype(jnp.float32)
    for d in range(1, n_tp):
        mix_copy(d).wait_recv()
        mixer = mixer + got[d].astype(jnp.float32)
    res[k, mine, :] = (tok[k].astype(jnp.float32) + mixer).astype(jnp.bfloat16)
    swap = to_pair(0, res.at[k, mine], res.at[k, mine])
    swapped = to_pair(0, res.at[k, theirs], res.at[k, theirs])
    swap.start()
    all_begin(0, mine)

    relay(order[2])
    all_middle(0, mine)
    swapped.wait_recv()
    all_begin(1, theirs)
    all_end(0, mine)
    norm(res, mine, ffn_gain)
    relay(order[3])
    all_middle(1, theirs)
    all_end(1, theirs)
    norm(res, theirs, ffn_gain)
    relay(order[4])

    def feed(t):
        arrived(("in", t))
        cut = pl.ds(pl.multiple_of(p * hidden_half + t * LANES, LANES), LANES)
        both = jnp.dot(normed[...], ffn_in[t, p], preferred_element_type=jnp.float32)
        both = both.astype(jnp.bfloat16).astype(jnp.float32)
        gate = conv_rows(both[:, :LANES], up_taps[0, :, cut], length) + up_bias[0:1, cut]
        value = conv_rows(both[:, LANES:], up_taps[1, :, cut], length) + up_bias[1:2, cut]
        units = (gate / (1.0 + jnp.exp(-gate)) * value).astype(jnp.bfloat16)
        hidden[:, pl.ds(pl.multiple_of(t * LANES, LANES), LANES)] = units

    beside = {0: 5, 1: 6, 3: 7}

    @pl.loop(0, n_in)
    def _(t):
        for at, index in beside.items():

            @pl.when(t == at)
            def _():
                relay(order[index])

        feed(t)

    def core_copy(u, dx):
        there = lax.rem(x + dx, n_x)
        return to_tp(
            part_ffn.at[u, :, there * 2 + 1 - c],
            got_core.at[u, :, there],
            core_send.at[u, dx],
            core_recv.at[u, dx],
            core,
        )

    def x_copy(u, dx):
        to = lax.rem(x + dx, n_x) * 2 + c
        return to_tp(sum_x.at[u, dx], got_x.at[u, dx], x_send.at[u, dx], x_recv.at[u, dx], to)

    def back(u):
        return to_pair(1 + u, sum_z.at[u], got_z.at[u])

    def chip_sum(u, o, dx):
        there = lax.rem(x + dx, n_x)
        mine_there = part_ffn[u, o, there * 2 + c].astype(jnp.float32)
        return mine_there + got_core[u, o, there].astype(jnp.float32)

    def place_sum(u, o):
        value = chip_sum(u, o, 0)
        for dx in range(1, n_x):
            value = value + got_x[u, dx, o].astype(jnp.float32)
        return value

    def down(u):
        arrived(("out", u))
        for o, at in enumerate((theirs, mine)):
            terms = jnp.dot(hidden[at, :], ffn_out[u, p], preferred_element_type=jnp.float32)
            for b in range(n_tp):
                part_ffn[u, o, b] = terms[:, b * LANES : (b + 1) * LANES].astype(jnp.bfloat16)
        for dx in (*range(1, n_x), 0):
            core_copy(u, dx).start()

    def over_x(u):
        for dx in range(1, n_x):
            core_copy(u, dx).wait_recv()
            for o in (0, 1):
                sum_x[u, dx, o] = chip_sum(u, o, dx).astype(jnp.bfloat16)
            x_copy(u, dx).start()

    def over_z(u):
        core_copy(u, 0).wait_recv()
        for dx in range(1, n_x):
            x_copy(u, dx).wait_recv()
        sum_z[u] = place_sum(u, 0).astype(jnp.bfloat16)
        back(u).start()

    for u in range(n_out):
        if 8 + u < len(order):
            relay(order[8 + u])
        down(u)
        if u >= 1:
            over_x(u - 1)
        if u >= 2:
            over_z(u - 2)
    over_x(n_out - 1)
    for u in range(max(n_out - 2, 0), n_out):
        over_z(u)
    for u in range(n_out):
        cut = slice(u * LANES, (u + 1) * LANES)
        value = res[k, mine, cut].astype(jnp.float32) + place_sum(u, 1)
        back(u).wait_recv()
        out[:, cut] = (value + got_z[u].astype(jnp.float32)).astype(jnp.bfloat16)

    for d in range(1, n_tp):
        tok_copy(d, k).wait_send()
        mix_copy(d).wait_send()
    for o, at in enumerate((mine, theirs)):
        wait_send(all_copies(o, at, "over"))
        wait_send(all_copies(o, at, "pass"))
    for u in range(n_out):
        for dx in range(n_x):
            core_copy(u, dx).wait_send()
        for dx in range(1, n_x):
            x_copy(u, dx).wait_send()
        back(u).wait_send()
    swap.wait_send()

    def drain(s):
        for q in chunks(s):
            for d in range(n_fs):
                for way, source in ((UP, j - d), (DOWN, j + d)):

                    @pl.when(comes(q, source, way) & goes_on(q, way))
                    def _():
                        wait_send(z_copies(s, q, source, way))

        q = None if s[0] == "mix" else p
        for d in range(1, n_fs):
            wait_send(y_copies(s, q, lax.rem(j + d, n_fs), g))

    drain(mix)

    @pl.loop(0, n_in)
    def _(t):
        drain(("in", t))

    @pl.loop(0, n_out)
    def _(u):
        drain(("out", u))


def fused(n_fs, n_tp, *args):
    tokens, w_signal, w_gate = args[0], args[2], args[8]
    rows, cols = tokens.shape
    shard, chans = w_signal.shape
    hidden = w_gate.shape[1] // 2
    n_in, n_out = hidden // LANES, shard // LANES
    width = n_fs * shard
    args = list(args)
    args[1], args[7] = args[1].reshape(1, -1), args[7].reshape(1, -1)
    in_vmem = {1, 5, 7, 10, 11}
    n_x = n_tp // 2
    copies = 2 + 2 * (n_in + n_out)
    dma = pltpu.SemaphoreType.DMA

    def held(*shape):
        return pltpu.VMEM(shape, jnp.bfloat16)

    return pl.pallas_call(
        functools.partial(layer_kernel, n_fs, n_tp),
        out_shape=jax.ShapeDtypeStruct((rows, cols), jnp.bfloat16),
        in_specs=[
            pl.BlockSpec(memory_space=pltpu.VMEM if i in in_vmem else pl.ANY)
            for i in range(len(args))
        ],
        out_specs=pl.BlockSpec(memory_space=pltpu.VMEM),
        scratch_shapes=[
            held(3, width, chans),
            held(n_fs, chans, shard),
            held(n_in, 2, width, 2 * LANES),
            held(n_out, 2, hidden, n_fs * LANES),
            held(n_tp, rows, cols),
            held(n_tp, 2 * rows, cols),
            held(2 * rows, width),
            held(2 * rows, hidden),
            held(n_tp, rows, cols),
            held(n_tp, rows, cols),
            held(n_out, 2, n_tp, rows, LANES),
            held(n_out, 2, n_x, rows, LANES),
            held(n_out, n_x, 2, rows, LANES),
            held(n_out, n_x, 2, rows, LANES),
            held(n_out, rows, LANES),
            held(n_out, rows, LANES),
            dma((2, copies, n_fs)),
            dma((copies, n_fs)),
            dma((copies, n_fs)),
            dma((copies, n_fs)),
            dma((5 + 4 * n_in + 2 * n_out,)),
            dma((2, n_tp)),
            dma((2, n_tp)),
            dma((2, 2, n_x)),
            dma((2, 2, n_x)),
            dma((n_out, n_x)),
            dma((n_out, n_x)),
            dma((n_out, n_x)),
            dma((n_out, n_x)),
            dma((1 + n_out,)),
            dma((1 + n_out,)),
        ],
        compiler_params=pltpu.CompilerParams(
            collective_id=0, has_side_effects=True, vmem_limit_bytes=62 * 1024 * 1024
        ),
    )(*args)


def solution(mesh):
    n_fs, n_tp = mesh.shape["fs"], mesh.shape["tp"]
    body = functools.partial(fused, n_fs, n_tp)
    if n_fs > 8 or n_fs != n_tp or n_fs % 2 or mesh.shape["grp"] != 2:
        body = on_device
    placed = (
        P(("grp", "fs"), "tp"),
        P(),
        P("fs", "tp"),
        P("fs", "tp"),
        P("fs", "tp"),
        P(None, "tp"),
        P("tp", "fs"),
        P(),
        P("fs", "tp"),
        P("fs", "tp"),
        P(None, None, "tp"),
        P(None, "tp"),
        P("tp", "fs"),
    )
    return jax.shard_map(
        body, mesh=mesh, in_specs=placed, out_specs=P(("grp", "fs"), "tp"), check_vma=False
    )
```
